32 devices in a mesh: sp: 8 (over z, y), dp: 4 (over x, core).
Axes of the slice: x: 2, y: 2, z: 4, core: 2. Of those that a mesh axis runs over, the one named last changes fastest.
Arguments:
- gated: bfloat16 [4, 1024, 3072], P('dp', 'sp'), may hold values from -6 to 6
- values_in: bfloat16 [4, 1024, 3072], P('dp', 'sp'), may hold values from -6 to 6
- upstream: bfloat16 [4, 1024, 3072], P('dp', 'sp'), may hold values from -6 to 6
- gain: float32 [3072], replicated, may hold values from 0.1 to 1.9
- shift: float32 [3072], replicated, may hold values from -3 to 3
- mix_w: bfloat16 [512, 4, 512], P('dp'), may hold values from -0.375 to 0.375
- mix_bias: float32 [4, 512], replicated, may hold values from 0.1 to 1.9
Outputs:
- grad_u: bfloat16 [4, 1024, 3072], P('dp', 'sp')
- grad_v: bfloat16 [4, 1024, 3072], P('dp', 'sp')
- grad_mix: float32 [512, 4, 512], P('dp')
- grad_bias: float32 [4, 512], replicated
- grad_gain: float32 [3072], replicated
- grad_shift: float32 [3072], replicated
The draws below stay inside these ranges and needn't reach their ends.
All inputs are finite; a program needn't handle non-finite values.
Results may differ from the reference program's by a relative error of at most 0.014.
Values may be sent and summed in bfloat16 or wider, within the bound.
A program may use at most 64 MiB of HBM per device.

```python
import jax
import jax.numpy as jnp
from jax import lax

GROUPS = 4
GROUP_DIM = 768
SPAN = 512
SEG = 64
HALF = 3072
LENGTH = 1024
BATCH = 4


def level_of(own_key, extent, shards, smallest, top_value):
    def one(dim, parts):
        steps = jax.random.uniform(jax.random.fold_in(jax.random.fold_in(own_key, 6), dim), (parts,), jnp.float32, smallest / len(shards), top_value / len(shards))
        return jnp.repeat(jnp.exp(steps), extent[dim] // parts).reshape((-1,) + (1,) * (len(extent) - dim - 1))

    loudness = one(*shards[0])
    for cut in shards[1:]:
        loudness = loudness * one(*cut)
    return loudness


def noise(rng, dims, deviation, most, split=(), kind=jnp.bfloat16):
    loudness = level_of(rng, dims, split, -0.22, 0.18) if split else 1.0
    drawn = jax.random.normal(rng, dims, jnp.float32) * deviation * loudness
    return jnp.minimum(jnp.maximum(drawn, -most), most).astype(kind)


def setup_inputs(seed: int = 0) -> dict:
    streams_of = jax.random.split(jax.random.key(seed), 8)
    gated = noise(streams_of[0], (BATCH, LENGTH, HALF), 1.0, 6.0, ((0, 4), (1, 8)))
    values_in = noise(streams_of[1], (BATCH, LENGTH, HALF), 1.0, 6.0, ((0, 4), (1, 8)))
    upstream = noise(streams_of[2], (BATCH, LENGTH, HALF), 1.0, 6.0, ((0, 4), (1, 8)))
    gain = jnp.clip(1.0 + 0.18 * jax.random.normal(streams_of[3], (HALF,), jnp.float32), 0.1, 1.9)
    shift = noise(streams_of[4], (HALF,), 0.5, 3.0, (), jnp.float32)
    mix_w = noise(streams_of[5], (SPAN, GROUPS, SPAN), (SPAN // 2) ** -0.5, 0.375, ((0, 4),))
    mix_bias = jnp.clip(1.0 + 0.18 * jax.random.normal(streams_of[6], (GROUPS, SPAN), jnp.float32), 0.1, 1.9)
    return {"gated": gated, "values_in": values_in, "upstream": upstream, "gain": gain, "shift": shift, "mix_w": mix_w, "mix_bias": mix_bias}


EPS = 1e-05

def span_mask():
    places = jnp.arange(SPAN)
    return (places[:, None] // SEG >= places[None, :] // SEG).astype(jnp.float32)

def reference(gated, values_in, upstream, gain, shift, mix_w, mix_bias):
    allowed = span_mask()
    masked_w = mix_w.astype(jnp.float32) * allowed[:, None, :]
    blocks = LENGTH // SPAN

    def one_sequence(carry, inputs):
        gated_row, values_row, upstream_row = inputs
        raw_values = values_row.astype(jnp.float32)
        centred = raw_values - lax.optimization_barrier(jnp.mean(raw_values, axis=-1, keepdims=True))
        inv_std = lax.rsqrt(lax.optimization_barrier(jnp.mean(centred * centred, axis=-1, keepdims=True)) + EPS)
        unit_v = centred * inv_std
        normed = (unit_v * gain + shift).astype(jnp.bfloat16)
        mix_grad = (upstream_row.astype(jnp.float32) * gated_row.astype(jnp.float32)).astype(jnp.bfloat16)
        norm_blocks = normed.reshape(blocks, SPAN, GROUPS, GROUP_DIM).astype(jnp.float32)
        grad_blocks = mix_grad.reshape(blocks, SPAN, GROUPS, GROUP_DIM).astype(jnp.float32)
        mixed_f = jnp.einsum('tgs,nsgc->ntgc', masked_w, norm_blocks) + mix_bias.T[None, :, :, None]
        mixed = lax.optimization_barrier(mixed_f.astype(jnp.bfloat16)).reshape(LENGTH, HALF)
        grad_u = (upstream_row.astype(jnp.float32) * mixed.astype(jnp.float32)).astype(jnp.bfloat16)
        back_f = jnp.einsum('tgs,ntgc->nsgc', masked_w, grad_blocks)
        grad_normed = lax.optimization_barrier(back_f.astype(jnp.bfloat16)).reshape(LENGTH, HALF).astype(jnp.float32)
        scaled = grad_normed * gain
        grad_v = inv_std * (scaled - lax.optimization_barrier(jnp.mean(scaled, axis=-1, keepdims=True)) - unit_v * lax.optimization_barrier(jnp.mean(scaled * unit_v, axis=-1, keepdims=True)))
        mix_term = jnp.einsum('ntgc,nsgc->tgs', grad_blocks, norm_blocks) * allowed[:, None, :]
        bias_term = lax.optimization_barrier(jnp.sum(grad_blocks, axis=(0, 3))).T
        carry = (carry[0] + mix_term, carry[1] + bias_term, carry[2] + lax.optimization_barrier(jnp.sum(grad_normed * unit_v, axis=0)), carry[3] + lax.optimization_barrier(jnp.sum(grad_normed, axis=0)))
        return (carry, (grad_u, grad_v.astype(jnp.bfloat16)))
    initial = (jnp.zeros((SPAN, GROUPS, SPAN), jnp.float32), jnp.zeros((GROUPS, SPAN), jnp.float32), jnp.zeros((HALF,), jnp.float32), jnp.zeros((HALF,), jnp.float32))
    totals, outputs = lax.scan(one_sequence, initial, (gated, values_in, upstream))
    return (outputs[0], outputs[1], totals[0], totals[1], totals[2], totals[3])
```

```python
import functools

import jax
import jax.numpy as jnp
from jax import lax
from jax.experimental import pallas as pl
from jax.experimental.pallas import tpu as pltpu
from jax.sharding import PartitionSpec as P

SEG = 64


EPS = 1e-05

CHUNK = 16


def kernel(
    dims,
    gated,
    values,
    upstream,
    gain,
    shift,
    mix_w,
    mix_bias,
    grad_u,
    grad_v,
    grad_mix,
    grad_bias,
    grad_gain,
    grad_shift,
    tok_g,
    tok_n,
    recv_g,
    recv_n,
    back_s,
    mixed_s,
    ret_b,
    ret_n,
    w_all,
    term_s,
    term_r,
    dp_sum,
    span_r,
    span_sum,
    group_r,
    acc_gain,
    acc_shift,
    vec_a,
    vec_b,
    vec_c,
    vec_s,
    bias_t,
    sq_send,
    sq_recv,
    dp_send,
    dp_recv,
    sn_send,
    sn_recv,
):
    tok, width, groups, span, dp_count, spans = dims
    half = groups * width
    rows = span // dp_count
    me = lax.axis_index("sp")
    my_span, k = me // groups, me % groups
    d = lax.axis_index("dp")
    f32, bf16 = jnp.float32, jnp.bfloat16

    def sq_id(j):
        return {"sp": my_span * groups + j}

    def dp_id(j):
        return {"dp": j}

    def sn_id(j):
        return {"sp": j * groups + k}

    class Exchange:
        def __init__(self, src, dst, own, count, where, send, recv, slot):
            self.src, self.dst, self.own, self.count = src, dst, own, count
            self.where, self.send, self.recv, self.slot = where, send, recv, slot

        def copy(self, step, to):
            peer = lax.rem(self.own + step, self.count)
            landing = self.own if to else peer
            return pltpu.make_async_remote_copy(
                src_ref=self.src(peer),
                dst_ref=self.dst(landing),
                send_sem=self.send.at[self.slot, step],
                recv_sem=self.recv.at[self.slot, landing],
                device_id=self.where(peer),
                device_id_type=pl.DeviceIdType.MESH,
            )

        def start(self):
            for step in range(1, self.count):
                self.copy(step, True).start()

        def arrive(self):
            for step in range(1, self.count):
                self.copy(step, False).wait_recv()

        def leave(self):
            for step in range(1, self.count):
                self.copy(step, True).wait_send()

    def square(src, dst, slot):
        return Exchange(src, dst, k, groups, sq_id, sq_send, sq_recv, slot)

    def across(src, dst, slot):
        return Exchange(src, dst, d, dp_count, dp_id, dp_send, dp_recv, slot)

    def spanning(src, dst, slot):
        return Exchange(src, dst, my_span, spans, sn_id, sn_send, sn_recv, slot)

    def w_rows(j):
        return w_all.at[pl.ds(pl.multiple_of(j * rows, rows), rows)]

    go_w = across(lambda j: mix_w.at[k], w_rows, 0)
    go_g = square(lambda j: tok_g.at[j], lambda j: recv_g.at[j], 0)
    go_n = square(lambda j: tok_n.at[j], lambda j: recv_n.at[j], 1)
    go_b = square(lambda j: back_s.at[j], lambda j: ret_b.at[j], 2)
    go_m = square(lambda j: mixed_s.at[j], lambda j: ret_n.at[j], 3)
    go_t = across(
        lambda j: term_s.at[pl.ds(pl.multiple_of(j * rows, rows), rows)],
        lambda j: term_r.at[j],
        1,
    )
    go_s = spanning(lambda j: dp_sum, lambda j: span_r.at[j], 0)
    go_q = square(lambda j: span_sum, lambda j: group_r.at[j], 4)
    go_va = across(lambda j: vec_s.at[0], lambda j: vec_a.at[j], 2)
    go_vb = square(lambda j: vec_s.at[1], lambda j: vec_b.at[j], 5)
    go_vc = spanning(lambda j: vec_s.at[2], lambda j: vec_c.at[j], 1)

    barrier = pltpu.get_barrier_semaphore()
    for own, count, where in ((k, groups, sq_id), (d, dp_count, dp_id), (my_span, spans, sn_id)):
        for step in range(1, count):
            pl.semaphore_signal(
                barrier,
                inc=1,
                device_id=where(lax.rem(own + step, count)),
                device_id_type=pl.DeviceIdType.MESH,
            )

    def piece(r):
        return pl.ds(pl.multiple_of(r * CHUNK, CHUNK), CHUNK)

    @pl.loop(0, tok // CHUNK)
    def _(r):
        at = piece(r)
        prod = (upstream[at, :].astype(f32) * gated[at, :].astype(f32)).astype(bf16)
        for g in range(groups):
            tok_g[g, at, :] = prod[:, g * width : (g + 1) * width]

    pl.semaphore_wait(barrier, groups + dp_count + spans - 3)
    go_w.start()
    go_g.start()

    def unit_of(at):
        raw = values[at, :].astype(f32)
        centred = raw - jnp.mean(raw, axis=-1, keepdims=True)
        inv_std = lax.rsqrt(jnp.mean(centred * centred, axis=-1, keepdims=True) + EPS)
        return centred * inv_std, inv_std

    @pl.loop(0, tok // CHUNK)
    def _(r):
        at = piece(r)
        unit, _inv = unit_of(at)
        normed = (unit * gain[...] + shift[...]).astype(bf16)
        for g in range(groups):
            tok_n[g, at, :] = normed[:, g * width : (g + 1) * width]

    go_n.start()
    w_rows(d)[...] = mix_w[k]
    recv_g[k] = tok_g[k]
    recv_n[k] = tok_n[k]
    acc_gain[...] = jnp.zeros_like(acc_gain)
    acc_shift[...] = jnp.zeros_like(acc_shift)
    bias_t[...] = jnp.transpose(jnp.broadcast_to(mix_bias[pl.ds(k, 1), :], (128, span)))

    def allowed(first, count):
        t = first + lax.broadcasted_iota(jnp.int32, (count, span), 0)
        s = lax.broadcasted_iota(jnp.int32, (count, span), 1)
        return lax.div(t, SEG) >= lax.div(s, SEG)

    go_w.arrive()
    for j in range(groups):
        at = slice(j * tok, (j + 1) * tok)
        w_all[at, :] = jnp.where(allowed(j * tok, tok), w_all[at, :].astype(f32), 0.0).astype(bf16)

    go_g.arrive()
    for j in range(groups):
        block = lax.dot_general(
            w_all[:, j * tok : (j + 1) * tok],
            recv_g[...].reshape(span, width),
            (((0,), (0,)), ((), ())),
            preferred_element_type=f32,
        )
        back_s[j] = block.astype(bf16)
    go_b.start()
    ret_b[k] = back_s[k]

    go_n.arrive()
    for j in range(groups):
        block = jnp.dot(
            w_all[j * tok : (j + 1) * tok, :],
            recv_n[...].reshape(span, width),
            preferred_element_type=f32,
        )
        bias = bias_t[j * tok : (j + 1) * tok, :]
        for c in range(width // 128):
            lanes = slice(c * 128, (c + 1) * 128)
            mixed_s[j, :, lanes] = (block[:, lanes] + bias).astype(bf16)
    go_m.start()
    ret_n[k] = mixed_s[k]

    for j in range(groups):
        block = lax.dot_general(
            recv_g[j],
            recv_n[...].reshape(span, width),
            (((1,), (1,)), ((), ())),
            preferred_element_type=f32,
        )
        term_s[j * tok : (j + 1) * tok, :] = jnp.where(allowed(j * tok, tok), block, 0.0).astype(bf16)
    go_t.start()
    term_r[d] = term_s[pl.ds(pl.multiple_of(d * rows, rows), rows), :]
    bias_sum = lax.dot_general(
        jnp.ones((8, width), bf16),
        recv_g[...].reshape(span, width),
        (((1,), (1,)), ((), ())),
        preferred_element_type=f32,
    )[0:1]

    go_b.arrive()

    @pl.loop(0, tok // CHUNK)
    def _(r):
        at = piece(r)
        unit, inv_std = unit_of(at)
        grad_normed = jnp.concatenate([ret_b[g, at, :] for g in range(groups)], axis=1).astype(f32)
        acc_gain[...] += grad_normed * unit
        acc_shift[...] += grad_normed
        scaled = grad_normed * gain[...]
        grad_v[at, :] = (
            inv_std
            * (
                scaled
                - jnp.mean(scaled, axis=-1, keepdims=True)
                - unit * jnp.mean(scaled * unit, axis=-1, keepdims=True)
            )
        ).astype(bf16)

    parts = half // span
    gain_sum = jnp.sum(acc_gain[...], axis=0, keepdims=True)
    shift_sum = jnp.sum(acc_shift[...], axis=0, keepdims=True)
    for i in range(parts):
        vec_s[0, i : i + 1, :] = gain_sum[:, i * span : (i + 1) * span]
        vec_s[0, parts + i : parts + i + 1, :] = shift_sum[:, i * span : (i + 1) * span]
    for g in range(groups):
        vec_s[0, 2 * parts + g : 2 * parts + g + 1, :] = jnp.where(k == g, bias_sum, 0.0)
    go_va.start()
    vec_a[d] = vec_s[0]

    def total(ref, count):
        out = ref[0].astype(f32)
        for i in range(1, count):
            out = out + ref[i].astype(f32)
        return out

    go_t.arrive()
    dp_sum[...] = total(term_r, dp_count).astype(bf16)
    go_s.start()
    span_r[my_span] = dp_sum[...]

    go_va.arrive()
    vec_s[1] = total(vec_a, dp_count)
    go_vb.start()
    vec_b[k] = vec_s[1]

    go_s.arrive()
    span_sum[...] = total(span_r, spans).astype(bf16)
    go_q.start()
    group_r[k] = span_sum[...]

    go_vb.arrive()
    vec_s[2] = total(vec_b, groups)
    go_vc.start()
    vec_c[my_span] = vec_s[2]

    go_m.arrive()

    @pl.loop(0, tok // CHUNK)
    def _(r):
        at = piece(r)
        mixed = jnp.concatenate([ret_n[g, at, :] for g in range(groups)], axis=1).astype(f32)
        grad_u[at, :] = (upstream[at, :].astype(f32) * mixed).astype(bf16)

    go_vc.arrive()
    summed = total(vec_c, spans)
    for i in range(parts):
        grad_gain[:, i * span : (i + 1) * span] = summed[i : i + 1, :]
        grad_shift[:, i * span : (i + 1) * span] = summed[parts + i : parts + i + 1, :]
    grad_bias[...] = summed[2 * parts : 2 * parts + groups, :]

    go_q.arrive()
    for g in range(groups):
        grad_mix[g] = group_r[g].astype(f32)

    for go in (go_w, go_g, go_n, go_b, go_m, go_t, go_s, go_q, go_va, go_vb, go_vc):
        go.leave()


def per_device(gated, values_in, upstream, gain, shift, mix_w, mix_bias):
    dp_count = lax.axis_size("dp")
    sp_count = lax.axis_size("sp")
    tok, half = gated.shape[1:]
    rows, groups, span = mix_w.shape
    width = half // groups
    assert span == groups * tok
    spans = sp_count // groups
    vec_rows = 2 * (half // span) + groups
    f32, bf16 = jnp.float32, jnp.bfloat16
    block = pltpu.VMEM((groups, tok, width), bf16)
    scratch = (
        [block] * 8
        + [
            pltpu.VMEM((span, span), bf16),
            pltpu.VMEM((span, span), bf16),
            pltpu.VMEM((dp_count, rows, span), bf16),
            pltpu.VMEM((rows, span), bf16),
            pltpu.VMEM((spans, rows, span), bf16),
            pltpu.VMEM((rows, span), bf16),
            pltpu.VMEM((groups, rows, span), bf16),
            pltpu.VMEM((CHUNK, half), f32),
            pltpu.VMEM((CHUNK, half), f32),
            pltpu.VMEM((dp_count, vec_rows, span), f32),
            pltpu.VMEM((groups, vec_rows, span), f32),
            pltpu.VMEM((spans, vec_rows, span), f32),
            pltpu.VMEM((3, vec_rows, span), f32),
            pltpu.VMEM((span, 128), f32),
        ]
        + [pltpu.SemaphoreType.DMA((6, groups))] * 2
        + [pltpu.SemaphoreType.DMA((3, dp_count))] * 2
        + [pltpu.SemaphoreType.DMA((2, spans))] * 2
    )
    vmem = pl.BlockSpec(memory_space=pltpu.VMEM)
    out = pl.pallas_call(
        functools.partial(kernel, (tok, width, groups, span, dp_count, spans)),
        out_shape=(
            jax.ShapeDtypeStruct((tok, half), bf16),
            jax.ShapeDtypeStruct((tok, half), bf16),
            jax.ShapeDtypeStruct((groups, rows, span), f32),
            jax.ShapeDtypeStruct((groups, span), f32),
            jax.ShapeDtypeStruct((1, half), f32),
            jax.ShapeDtypeStruct((1, half), f32),
        ),
        in_specs=[vmem] * 7,
        out_specs=[vmem] * 6,
        scratch_shapes=scratch,
        compiler_params=pltpu.CompilerParams(
            collective_id=0, has_side_effects=True, vmem_limit_bytes=48 * 1024 * 1024
        ),
    )(
        gated[0],
        values_in[0],
        upstream[0],
        gain[None],
        shift[None],
        jnp.transpose(mix_w, (1, 0, 2)),
        mix_bias,
    )
    return (
        out[0][None],
        out[1][None],
        jnp.transpose(out[2], (1, 0, 2)),
        out[3],
        out[4][0],
        out[5][0],
    )


def solution(mesh):
    placed = (
        P("dp", "sp", None),
        P("dp", "sp", None),
        P("dp", "sp", None),
        P(),
        P(),
        P("dp", None, None),
        P(),
    )
    return jax.shard_map(
        per_device,
        mesh=mesh,
        in_specs=placed,
        out_specs=(P("dp", "sp", None), P("dp", "sp", None), P("dp", None, None), P(), P(), P()),
        check_vma=False,
    )
```

```python
import functools

import jax
import jax.numpy as jnp
from jax import lax
from jax.experimental import pallas as pl
from jax.experimental.pallas import tpu as pltpu
from jax.sharding import PartitionSpec as P

SEG = 64


EPS = 1e-05

CHUNK = 16


def kernel(
    dims,
    gated_in,
    values_hbm,
    upstream_in,
    gain,
    shift,
    mix_w,
    mix_bias,
    grad_u,
    grad_v,
    group_r,
    summed,
    gated,
    values,
    upstream,
    my_w,
    tok_g,
    tok_n,
    recv_g,
    recv_n,
    back_s,
    mixed_s,
    ret_b,
    ret_n,
    w_all,
    term_s,
    term_r,
    dp_sum,
    span_r,
    span_sum,
    acc_gain,
    acc_shift,
    vec_a,
    vec_b,
    vec_c,
    vec_s,
    bias_t,
    sq_send,
    sq_recv,
    dp_send,
    dp_recv,
    sn_send,
    sn_recv,
    in_sem,
):
    tok, width, groups, span, dp_count, spans = dims
    half = groups * width
    rows = span // dp_count
    me = lax.axis_index("sp")
    my_span, k = me // groups, me % groups
    d = lax.axis_index("dp")
    f32, bf16 = jnp.float32, jnp.bfloat16

    def sq_id(j):
        return {"sp": my_span * groups + j}

    def dp_id(j):
        return {"dp": j}

    def sn_id(j):
        return {"sp": j * groups + k}

    class Exchange:
        def __init__(self, src, dst, own, count, where, send, recv, slot):
            self.src, self.dst, self.own, self.count = src, dst, own, count
            self.where, self.send, self.recv, self.slot = where, send, recv, slot

        def copy(self, step, to):
            peer = lax.rem(self.own + step, self.count)
            landing = self.own if to else peer
            return pltpu.make_async_remote_copy(
                src_ref=self.src(peer),
                dst_ref=self.dst(landing),
                send_sem=self.send.at[self.slot, step],
                recv_sem=self.recv.at[self.slot, landing],
                device_id=self.where(peer),
                device_id_type=pl.DeviceIdType.MESH,
            )

        def start(self):
            for step in range(1, self.count):
                self.copy(step, True).start()

        def arrive(self):
            for step in range(1, self.count):
                self.copy(step, False).wait_recv()

        def leave(self):
            for step in range(1, self.count):
                self.copy(step, True).wait_send()

    def square(src, dst, slot):
        return Exchange(src, dst, k, groups, sq_id, sq_send, sq_recv, slot)

    def across(src, dst, slot):
        return Exchange(src, dst, d, dp_count, dp_id, dp_send, dp_recv, slot)

    def spanning(src, dst, slot):
        return Exchange(src, dst, my_span, spans, sn_id, sn_send, sn_recv, slot)

    def w_rows(j):
        return w_all.at[pl.ds(pl.multiple_of(j * rows, rows), rows)]

    go_w = across(lambda j: my_w, w_rows, 0)
    go_g = square(lambda j: tok_g.at[j], lambda j: recv_g.at[j], 0)
    go_n = square(lambda j: tok_n.at[j], lambda j: recv_n.at[j], 1)
    go_b = square(lambda j: back_s.at[j], lambda j: ret_b.at[j], 2)
    go_m = square(lambda j: mixed_s.at[j], lambda j: ret_n.at[j], 3)
    go_t = across(
        lambda j: term_s.at[pl.ds(pl.multiple_of(j * rows, rows), rows)],
        lambda j: term_r.at[j],
        1,
    )
    go_s = spanning(lambda j: dp_sum, lambda j: span_r.at[j], 0)
    go_q = square(lambda j: span_sum, lambda j: group_r.at[j], 4)
    go_va = across(lambda j: vec_s.at[0], lambda j: vec_a.at[j], 2)
    go_vb = square(lambda j: vec_s.at[1], lambda j: vec_b.at[j], 5)
    go_vc = spanning(lambda j: vec_s.at[2], lambda j: vec_c.at[j], 1)

    fetches = [
        pltpu.make_async_copy(src, dst, in_sem.at[i])
        for i, (src, dst) in enumerate(
            ((gated_in, gated), (upstream_in, upstream), (values_hbm, values))
        )
    ]
    for fetch in fetches:
        fetch.start()

    barrier = pltpu.get_barrier_semaphore()
    for own, count, where in ((k, groups, sq_id), (d, dp_count, dp_id), (my_span, spans, sn_id)):
        for step in range(1, count):
            pl.semaphore_signal(
                barrier,
                inc=1,
                device_id=where(lax.rem(own + step, count)),
                device_id_type=pl.DeviceIdType.MESH,
            )

    def piece(r):
        return pl.ds(pl.multiple_of(r * CHUNK, CHUNK), CHUNK)

    fetches[0].wait()
    fetches[1].wait()

    @pl.loop(0, tok // CHUNK)
    def _(r):
        at = piece(r)
        prod = (upstream[at, :].astype(f32) * gated[at, :].astype(f32)).astype(bf16)
        for g in range(groups):
            tok_g[g, at, :] = prod[:, g * width : (g + 1) * width]

    pl.semaphore_wait(barrier, groups + dp_count + spans - 3)
    go_g.start()

    @pl.loop(0, rows // CHUNK)
    def _(r):
        at = piece(r)
        whole = mix_w[at].astype(f32)
        rows_of = whole[:, 0, :]
        for g in range(1, groups):
            rows_of = jnp.where(k == g, whole[:, g, :], rows_of)
        my_w[at, :] = rows_of.astype(bf16)

    go_w.start()
    fetches[2].wait()

    def unit_of(at):
        raw = values[at, :].astype(f32)
        centred = raw - jnp.mean(raw, axis=-1, keepdims=True)
        inv_std = lax.rsqrt(jnp.mean(centred * centred, axis=-1, keepdims=True) + EPS)
        return centred * inv_std, inv_std

    @pl.loop(0, tok // CHUNK)
    def _(r):
        at = piece(r)
        unit, _inv = unit_of(at)
        normed = (unit * gain[...] + shift[...]).astype(bf16)
        for g in range(groups):
            tok_n[g, at, :] = normed[:, g * width : (g + 1) * width]

    go_n.start()
    w_rows(d)[...] = my_w[...]
    recv_g[k] = tok_g[k]
    recv_n[k] = tok_n[k]
    acc_gain[...] = jnp.zeros_like(acc_gain)
    acc_shift[...] = jnp.zeros_like(acc_shift)
    bias_t[...] = jnp.transpose(jnp.broadcast_to(mix_bias[pl.ds(k, 1), :], (128, span)))

    def allowed(first, count):
        t = first + lax.broadcasted_iota(jnp.int32, (count, span), 0)
        s = lax.broadcasted_iota(jnp.int32, (count, span), 1)
        return lax.div(t, SEG) >= lax.div(s, SEG)

    go_w.arrive()
    for j in range(groups):
        at = slice(j * tok, (j + 1) * tok)
        w_all[at, :] = jnp.where(allowed(j * tok, tok), w_all[at, :].astype(f32), 0.0).astype(bf16)

    go_g.arrive()
    for j in range(groups):
        block = lax.dot_general(
            w_all[:, j * tok : (j + 1) * tok],
            recv_g[...].reshape(span, width),
            (((0,), (0,)), ((), ())),
            preferred_element_type=f32,
        )
        back_s[j] = block.astype(bf16)
    go_b.start()
    ret_b[k] = back_s[k]

    go_n.arrive()
    for j in range(groups):
        block = lax.dot_general(
            recv_g[j],
            recv_n[...].reshape(span, width),
            (((1,), (1,)), ((), ())),
            preferred_element_type=f32,
        )
        term_s[j * tok : (j + 1) * tok, :] = jnp.where(allowed(j * tok, tok), block, 0.0).astype(bf16)
    go_t.start()
    term_r[d] = term_s[pl.ds(pl.multiple_of(d * rows, rows), rows), :]
    for j in range(groups):
        block = jnp.dot(
            w_all[j * tok : (j + 1) * tok, :],
            recv_n[...].reshape(span, width),
            preferred_element_type=f32,
        )
        bias = bias_t[j * tok : (j + 1) * tok, :]
        for c in range(width // 128):
            lanes = slice(c * 128, (c + 1) * 128)
            mixed_s[j, :, lanes] = (block[:, lanes] + bias).astype(bf16)
    go_m.start()
    ret_n[k] = mixed_s[k]

    bias_sum = lax.dot_general(
        jnp.ones((8, width), bf16),
        recv_g[...].reshape(span, width),
        (((1,), (1,)), ((), ())),
        preferred_element_type=f32,
    )[0:1]

    go_b.arrive()

    @pl.loop(0, tok // CHUNK)
    def _(r):
        at = piece(r)
        unit, inv_std = unit_of(at)
        grad_normed = jnp.concatenate([ret_b[g, at, :] for g in range(groups)], axis=1).astype(f32)
        acc_gain[...] += grad_normed * unit
        acc_shift[...] += grad_normed
        scaled = grad_normed * gain[...]
        grad_v[at, :] = (
            inv_std
            * (
                scaled
                - jnp.mean(scaled, axis=-1, keepdims=True)
                - unit * jnp.mean(scaled * unit, axis=-1, keepdims=True)
            )
        ).astype(bf16)

    parts = half // span
    gain_sum = jnp.sum(acc_gain[...], axis=0, keepdims=True)
    shift_sum = jnp.sum(acc_shift[...], axis=0, keepdims=True)
    for i in range(parts):
        vec_s[0, i : i + 1, :] = gain_sum[:, i * span : (i + 1) * span]
        vec_s[0, parts + i : parts + i + 1, :] = shift_sum[:, i * span : (i + 1) * span]
    for g in range(groups):
        vec_s[0, 2 * parts + g : 2 * parts + g + 1, :] = jnp.where(k == g, bias_sum, 0.0)
    go_va.start()
    vec_a[d] = vec_s[0]

    def total(ref, count):
        out = ref[0].astype(f32)
        for i in range(1, count):
            out = out + ref[i].astype(f32)
        return out

    go_t.arrive()
    dp_sum[...] = total(term_r, dp_count).astype(bf16)
    go_s.start()
    span_r[my_span] = dp_sum[...]

    go_va.arrive()
    vec_s[1] = total(vec_a, dp_count)
    go_vb.start()
    vec_b[k] = vec_s[1]

    go_s.arrive()
    span_sum[...] = total(span_r, spans).astype(bf16)
    go_q.start()
    group_r[k] = span_sum[...]

    go_vb.arrive()
    vec_s[2] = total(vec_b, groups)
    go_vc.start()
    vec_c[my_span] = vec_s[2]

    go_m.arrive()

    @pl.loop(0, tok // CHUNK)
    def _(r):
        at = piece(r)
        mixed = jnp.concatenate([ret_n[g, at, :] for g in range(groups)], axis=1).astype(f32)
        grad_u[at, :] = (upstream[at, :].astype(f32) * mixed).astype(bf16)

    go_vc.arrive()
    summed[...] = total(vec_c, spans)
    go_q.arrive()

    for go in (go_w, go_g, go_n, go_b, go_m, go_t, go_s, go_q, go_va, go_vb, go_vc):
        go.leave()


def finish(
    u_in, v_in, group_r, summed, grad_u, grad_v, grad_mix, grad_bias, grad_gain, grad_shift, sems
):
    copies = [
        pltpu.make_async_copy(u_in, grad_u, sems.at[0]),
        pltpu.make_async_copy(v_in, grad_v, sems.at[1]),
    ]
    for copy in copies:
        copy.start()
    groups, span = grad_bias.shape
    parts = grad_gain.shape[-1] // span
    for g in range(groups):
        grad_mix[:, g, :] = group_r[g].astype(jnp.float32)
    for i in range(parts):
        grad_gain[:, i * span : (i + 1) * span] = summed[i : i + 1, :]
        grad_shift[:, i * span : (i + 1) * span] = summed[parts + i : parts + i + 1, :]
    grad_bias[...] = summed[2 * parts : 2 * parts + groups, :]
    for copy in copies:
        copy.wait()


def per_device(gated, values_in, upstream, gain, shift, mix_w, mix_bias):
    dp_count = lax.axis_size("dp")
    sp_count = lax.axis_size("sp")
    tok, half = gated.shape[1:]
    rows, groups, span = mix_w.shape
    width = half // groups
    assert span == groups * tok
    spans = sp_count // groups
    vec_rows = 2 * (half // span) + groups
    f32, bf16 = jnp.float32, jnp.bfloat16
    block = pltpu.VMEM((groups, tok, width), bf16)
    hbm = pl.BlockSpec(memory_space=pltpu.HBM)
    scratch = (
        [pltpu.VMEM((tok, half), bf16)] * 3
        + [pltpu.VMEM((rows, span), bf16)]
        + [block] * 8
        + [
            pltpu.VMEM((span, span), bf16),
            pltpu.VMEM((span, span), bf16),
            pltpu.VMEM((dp_count, rows, span), bf16),
            pltpu.VMEM((rows, span), bf16),
            pltpu.VMEM((spans, rows, span), bf16),
            pltpu.VMEM((rows, span), bf16),
            pltpu.VMEM((CHUNK, half), f32),
            pltpu.VMEM((CHUNK, half), f32),
            pltpu.VMEM((dp_count, vec_rows, span), f32),
            pltpu.VMEM((groups, vec_rows, span), f32),
            pltpu.VMEM((spans, vec_rows, span), f32),
            pltpu.VMEM((3, vec_rows, span), f32),
            pltpu.VMEM((span, 128), f32),
        ]
        + [pltpu.SemaphoreType.DMA((6, groups))] * 2
        + [pltpu.SemaphoreType.DMA((3, dp_count))] * 2
        + [pltpu.SemaphoreType.DMA((2, spans))] * 2
        + [pltpu.SemaphoreType.DMA((3,))]
    )
    vmem = pl.BlockSpec(memory_space=pltpu.VMEM)
    out = pl.pallas_call(
        functools.partial(kernel, (tok, width, groups, span, dp_count, spans)),
        out_shape=(
            jax.ShapeDtypeStruct((tok, half), bf16),
            jax.ShapeDtypeStruct((tok, half), bf16),
            jax.ShapeDtypeStruct((groups, rows, span), bf16),
            jax.ShapeDtypeStruct((vec_rows, span), f32),
        ),
        in_specs=[hbm] * 3 + [vmem] * 4,
        out_specs=[vmem] * 4,
        scratch_shapes=scratch,
        compiler_params=pltpu.CompilerParams(
            collective_id=0, has_side_effects=True, vmem_limit_bytes=60 * 1024 * 1024
        ),
    )(
        gated[0],
        values_in[0],
        upstream[0],
        gain[None],
        shift[None],
        mix_w,
        mix_bias,
    )
    u, v, mix, bias, gain_g, shift_g = pl.pallas_call(
        finish,
        out_shape=(
            jax.ShapeDtypeStruct((tok, half), bf16),
            jax.ShapeDtypeStruct((tok, half), bf16),
            jax.ShapeDtypeStruct((rows, groups, span), f32),
            jax.ShapeDtypeStruct((groups, span), f32),
            jax.ShapeDtypeStruct((1, half), f32),
            jax.ShapeDtypeStruct((1, half), f32),
        ),
        in_specs=[vmem] * 4,
        out_specs=[hbm] * 2 + [vmem] * 4,
        scratch_shapes=[pltpu.SemaphoreType.DMA((2,))],
        compiler_params=pltpu.CompilerParams(vmem_limit_bytes=60 * 1024 * 1024),
    )(*out)
    return (u[None], v[None], mix, bias, gain_g[0], shift_g[0])


def solution(mesh):
    placed = (
        P("dp", "sp", None),
        P("dp", "sp", None),
        P("dp", "sp", None),
        P(),
        P(),
        P("dp", None, None),
        P(),
    )
    return jax.shard_map(
        per_device,
        mesh=mesh,
        in_specs=placed,
        out_specs=(P("dp", "sp", None), P("dp", "sp", None), P("dp", None, None), P(), P(), P()),
        check_vma=False,
    )
```

```python
import functools

import jax
import jax.numpy as jnp
from jax import lax
from jax.experimental import pallas as pl
from jax.experimental.pallas import tpu as pltpu
from jax.sharding import PartitionSpec as P

SEG = 64


EPS = 1e-05

CHUNK = 16


def kernel(
    dims,
    gated_in,
    values_hbm,
    upstream_in,
    gain,
    shift,
    mix_w,
    mix_bias,
    grad_u,
    grad_v,
    group_r,
    summed,
    gated,
    values,
    upstream,
    my_w,
    tok_g,
    tok_n,
    recv_g,
    recv_n,
    back_s,
    mixed_s,
    ret_b,
    ret_n,
    w_all,
    term_s,
    term_r,
    dp_sum,
    span_r,
    span_sum,
    acc_gain,
    acc_shift,
    vec_a,
    vec_b,
    vec_c,
    vec_s,
    bias_t,
    sq_send,
    sq_recv,
    dp_send,
    dp_recv,
    sn_send,
    sn_recv,
    in_sem,
):
    tok, width, groups, span, dp_count, spans = dims
    half = groups * width
    rows = span // dp_count
    me = lax.axis_index("sp")
    my_span, k = me // groups, me % groups
    d = lax.axis_index("dp")
    f32, bf16 = jnp.float32, jnp.bfloat16

    def sq_id(j):
        return {"sp": my_span * groups + j}

    def dp_id(j):
        return {"dp": j}

    def sn_id(j):
        return {"sp": j * groups + k}

    class Exchange:
        def __init__(self, src, dst, own, count, where, send, recv, slot):
            self.src, self.dst, self.own, self.count = src, dst, own, count
            self.where, self.send, self.recv, self.slot = where, send, recv, slot

        def copy(self, step, to):
            peer = lax.rem(self.own + step, self.count)
            landing = self.own if to else peer
            return pltpu.make_async_remote_copy(
                src_ref=self.src(peer),
                dst_ref=self.dst(landing),
                send_sem=self.send.at[self.slot, step],
                recv_sem=self.recv.at[self.slot, landing],
                device_id=self.where(peer),
                device_id_type=pl.DeviceIdType.MESH,
            )

        def start(self):
            for step in range(1, self.count):
                self.copy(step, True).start()

        def arrive(self):
            for step in range(1, self.count):
                self.copy(step, False).wait_recv()

        def leave(self):
            for step in range(1, self.count):
                self.copy(step, True).wait_send()

    def square(src, dst, slot):
        return Exchange(src, dst, k, groups, sq_id, sq_send, sq_recv, slot)

    def across(src, dst, slot):
        return Exchange(src, dst, d, dp_count, dp_id, dp_send, dp_recv, slot)

    def spanning(src, dst, slot):
        return Exchange(src, dst, my_span, spans, sn_id, sn_send, sn_recv, slot)

    def w_rows(j):
        return w_all.at[pl.ds(pl.multiple_of(j * rows, rows), rows)]

    go_w = across(lambda j: my_w, w_rows, 0)
    go_g = square(lambda j: tok_g.at[j], lambda j: recv_g.at[j], 0)
    go_n = square(lambda j: tok_n.at[j], lambda j: recv_n.at[j], 1)
    go_b = square(lambda j: back_s.at[j], lambda j: ret_b.at[j], 2)
    go_m = square(lambda j: mixed_s.at[j], lambda j: ret_n.at[j], 3)
    go_t = across(
        lambda j: term_s.at[pl.ds(pl.multiple_of(j * rows, rows), rows)],
        lambda j: term_r.at[j],
        1,
    )
    go_s = spanning(lambda j: dp_sum, lambda j: span_r.at[j], 0)
    go_q = square(lambda j: span_sum, lambda j: group_r.at[j], 4)
    go_va = across(lambda j: vec_s.at[0], lambda j: vec_a.at[j], 2)
    go_vb = square(lambda j: vec_s.at[1], lambda j: vec_b.at[j], 5)
    go_vc = spanning(lambda j: vec_s.at[2], lambda j: vec_c.at[j], 1)

    fetches = [
        pltpu.make_async_copy(src, dst, in_sem.at[i])
        for i, (src, dst) in enumerate(
            ((gated_in, gated), (upstream_in, upstream), (values_hbm, values))
        )
    ]
    for fetch in fetches:
        fetch.start()

    barrier = pltpu.get_barrier_semaphore()
    for own, count, where in ((k, groups, sq_id), (d, dp_count, dp_id), (my_span, spans, sn_id)):
        for step in range(1, count):
            pl.semaphore_signal(
                barrier,
                inc=1,
                device_id=where(lax.rem(own + step, count)),
                device_id_type=pl.DeviceIdType.MESH,
            )

    def piece(r):
        return pl.ds(pl.multiple_of(r * CHUNK, CHUNK), CHUNK)

    fetches[0].wait()
    fetches[1].wait()

    @pl.loop(0, tok // CHUNK)
    def _(r):
        at = piece(r)
        prod = (upstream[at, :].astype(f32) * gated[at, :].astype(f32)).astype(bf16)
        for g in range(groups):
            tok_g[g, at, :] = prod[:, g * width : (g + 1) * width]

    pl.semaphore_wait(barrier, groups + dp_count + spans - 3)
    go_g.start()

    @pl.loop(0, rows // CHUNK)
    def _(r):
        at = piece(r)
        whole = mix_w[at].astype(f32)
        rows_of = whole[:, 0, :]
        for g in range(1, groups):
            rows_of = jnp.where(k == g, whole[:, g, :], rows_of)
        my_w[at, :] = rows_of.astype(bf16)

    go_w.start()
    fetches[2].wait()

    def unit_of(at):
        raw = values[at, :].astype(f32)
        centred = raw - jnp.mean(raw, axis=-1, keepdims=True)
        inv_std = lax.rsqrt(jnp.mean(centred * centred, axis=-1, keepdims=True) + EPS)
        return centred * inv_std, inv_std

    @pl.loop(0, tok // CHUNK)
    def _(r):
        at = piece(r)
        unit, _inv = unit_of(at)
        normed = (unit * gain[...] + shift[...]).astype(bf16)
        for g in range(groups):
            tok_n[g, at, :] = normed[:, g * width : (g + 1) * width]

    go_n.start()
    w_rows(d)[...] = my_w[...]
    recv_g[k] = tok_g[k]
    recv_n[k] = tok_n[k]
    acc_gain[...] = jnp.zeros_like(acc_gain)
    acc_shift[...] = jnp.zeros_like(acc_shift)
    bias_t[...] = jnp.transpose(jnp.broadcast_to(mix_bias[pl.ds(k, 1), :], (128, span)))

    def allowed(first, count):
        t = first + lax.broadcasted_iota(jnp.int32, (count, span), 0)
        s = lax.broadcasted_iota(jnp.int32, (count, span), 1)
        return lax.div(t, SEG) >= lax.div(s, SEG)

    go_w.arrive()
    for j in range(groups):
        at = slice(j * tok, (j + 1) * tok)
        w_all[at, :] = jnp.where(allowed(j * tok, tok), w_all[at, :].astype(f32), 0.0).astype(bf16)

    go_g.arrive()
    for j in range(groups):
        block = lax.dot_general(
            w_all[:, j * tok : (j + 1) * tok],
            recv_g[...].reshape(span, width),
            (((0,), (0,)), ((), ())),
            preferred_element_type=f32,
        )
        back_s[j] = block.astype(bf16)
    go_b.start()
    ret_b[k] = back_s[k]

    go_n.arrive()
    for j in range(groups):
        block = lax.dot_general(
            recv_g[j],
            recv_n[...].reshape(span, width),
            (((1,), (1,)), ((), ())),
            preferred_element_type=f32,
        )
        term_s[j * tok : (j + 1) * tok, :] = jnp.where(allowed(j * tok, tok), block, 0.0).astype(bf16)
    go_t.start()
    term_r[d] = term_s[pl.ds(pl.multiple_of(d * rows, rows), rows), :]
    for j in range(groups):
        block = jnp.dot(
            w_all[j * tok : (j + 1) * tok, :],
            recv_n[...].reshape(span, width),
            preferred_element_type=f32,
        )
        bias = bias_t[j * tok : (j + 1) * tok, :]
        for c in range(width // 128):
            lanes = slice(c * 128, (c + 1) * 128)
            mixed_s[j, :, lanes] = (block[:, lanes] + bias).astype(bf16)
    go_m.start()
    ret_n[k] = mixed_s[k]

    bias_sum = lax.dot_general(
        jnp.ones((8, width), bf16),
        recv_g[...].reshape(span, width),
        (((1,), (1,)), ((), ())),
        preferred_element_type=f32,
    )[0:1]

    def total(ref, count):
        out = ref[0].astype(f32)
        for i in range(1, count):
            out = out + ref[i].astype(f32)
        return out

    go_t.arrive()
    dp_sum[...] = total(term_r, dp_count).astype(bf16)
    go_s.start()
    span_r[my_span] = dp_sum[...]

    go_b.arrive()

    @pl.loop(0, tok // CHUNK)
    def _(r):
        at = piece(r)
        unit, inv_std = unit_of(at)
        grad_normed = jnp.concatenate([ret_b[g, at, :] for g in range(groups)], axis=1).astype(f32)
        acc_gain[...] += grad_normed * unit
        acc_shift[...] += grad_normed
        scaled = grad_normed * gain[...]
        grad_v[at, :] = (
            inv_std
            * (
                scaled
                - jnp.mean(scaled, axis=-1, keepdims=True)
                - unit * jnp.mean(scaled * unit, axis=-1, keepdims=True)
            )
        ).astype(bf16)

    parts = half // span
    gain_sum = jnp.sum(acc_gain[...], axis=0, keepdims=True)
    shift_sum = jnp.sum(acc_shift[...], axis=0, keepdims=True)
    for i in range(parts):
        vec_s[0, i : i + 1, :] = gain_sum[:, i * span : (i + 1) * span]
        vec_s[0, parts + i : parts + i + 1, :] = shift_sum[:, i * span : (i + 1) * span]
    for g in range(groups):
        vec_s[0, 2 * parts + g : 2 * parts + g + 1, :] = jnp.where(k == g, bias_sum, 0.0)
    go_va.start()
    vec_a[d] = vec_s[0]

    go_va.arrive()
    vec_s[1] = total(vec_a, dp_count)
    go_vb.start()
    vec_b[k] = vec_s[1]

    go_s.arrive()
    span_sum[...] = total(span_r, spans).astype(bf16)
    go_q.start()
    group_r[k] = span_sum[...]

    go_vb.arrive()
    vec_s[2] = total(vec_b, groups)
    go_vc.start()
    vec_c[my_span] = vec_s[2]

    go_m.arrive()

    @pl.loop(0, tok // CHUNK)
    def _(r):
        at = piece(r)
        mixed = jnp.concatenate([ret_n[g, at, :] for g in range(groups)], axis=1).astype(f32)
        grad_u[at, :] = (upstream[at, :].astype(f32) * mixed).astype(bf16)

    go_vc.arrive()
    summed[...] = total(vec_c, spans)
    go_q.arrive()

    for go in (go_w, go_g, go_n, go_b, go_m, go_t, go_s, go_q, go_va, go_vb, go_vc):
        go.leave()


def finish(
    u_in, v_in, group_r, summed, grad_u, grad_v, grad_mix, grad_bias, grad_gain, grad_shift, sems
):
    copies = [
        pltpu.make_async_copy(u_in, grad_u, sems.at[0]),
        pltpu.make_async_copy(v_in, grad_v, sems.at[1]),
    ]
    for copy in copies:
        copy.start()
    groups, span = grad_bias.shape
    parts = grad_gain.shape[-1] // span
    for g in range(groups):
        grad_mix[:, g, :] = group_r[g].astype(jnp.float32)
    for i in range(parts):
        grad_gain[:, i * span : (i + 1) * span] = summed[i : i + 1, :]
        grad_shift[:, i * span : (i + 1) * span] = summed[parts + i : parts + i + 1, :]
    grad_bias[...] = summed[2 * parts : 2 * parts + groups, :]
    for copy in copies:
        copy.wait()


def per_device(gated, values_in, upstream, gain, shift, mix_w, mix_bias):
    dp_count = lax.axis_size("dp")
    sp_count = lax.axis_size("sp")
    tok, half = gated.shape[1:]
    rows, groups, span = mix_w.shape
    width = half // groups
    assert span == groups * tok
    spans = sp_count // groups
    vec_rows = 2 * (half // span) + groups
    f32, bf16 = jnp.float32, jnp.bfloat16
    block = pltpu.VMEM((groups, tok, width), bf16)
    hbm = pl.BlockSpec(memory_space=pltpu.HBM)
    scratch = (
        [pltpu.VMEM((tok, half), bf16)] * 3
        + [pltpu.VMEM((rows, span), bf16)]
        + [block] * 8
        + [
            pltpu.VMEM((span, span), bf16),
            pltpu.VMEM((span, span), bf16),
            pltpu.VMEM((dp_count, rows, span), bf16),
            pltpu.VMEM((rows, span), bf16),
            pltpu.VMEM((spans, rows, span), bf16),
            pltpu.VMEM((rows, span), bf16),
            pltpu.VMEM((CHUNK, half), f32),
            pltpu.VMEM((CHUNK, half), f32),
            pltpu.VMEM((dp_count, vec_rows, span), f32),
            pltpu.VMEM((groups, vec_rows, span), f32),
            pltpu.VMEM((spans, vec_rows, span), f32),
            pltpu.VMEM((3, vec_rows, span), f32),
            pltpu.VMEM((span, 128), f32),
        ]
        + [pltpu.SemaphoreType.DMA((6, groups))] * 2
        + [pltpu.SemaphoreType.DMA((3, dp_count))] * 2
        + [pltpu.SemaphoreType.DMA((2, spans))] * 2
        + [pltpu.SemaphoreType.DMA((3,))]
    )
    vmem = pl.BlockSpec(memory_space=pltpu.VMEM)
    out = pl.pallas_call(
        functools.partial(kernel, (tok, width, groups, span, dp_count, spans)),
        out_shape=(
            jax.ShapeDtypeStruct((tok, half), bf16),
            jax.ShapeDtypeStruct((tok, half), bf16),
            jax.ShapeDtypeStruct((groups, rows, span), bf16),
            jax.ShapeDtypeStruct((vec_rows, span), f32),
        ),
        in_specs=[hbm] * 3 + [vmem] * 4,
        out_specs=[vmem] * 4,
        scratch_shapes=scratch,
        compiler_params=pltpu.CompilerParams(
            collective_id=0, has_side_effects=True, vmem_limit_bytes=60 * 1024 * 1024
        ),
    )(
        gated[0],
        values_in[0],
        upstream[0],
        gain[None],
        shift[None],
        mix_w,
        mix_bias,
    )
    u, v, mix, bias, gain_g, shift_g = pl.pallas_call(
        finish,
        out_shape=(
            jax.ShapeDtypeStruct((tok, half), bf16),
            jax.ShapeDtypeStruct((tok, half), bf16),
            jax.ShapeDtypeStruct((rows, groups, span), f32),
            jax.ShapeDtypeStruct((groups, span), f32),
            jax.ShapeDtypeStruct((1, half), f32),
            jax.ShapeDtypeStruct((1, half), f32),
        ),
        in_specs=[vmem] * 4,
        out_specs=[hbm] * 2 + [vmem] * 4,
        scratch_shapes=[pltpu.SemaphoreType.DMA((2,))],
        compiler_params=pltpu.CompilerParams(vmem_limit_bytes=60 * 1024 * 1024),
    )(*out)
    return (u[None], v[None], mix, bias, gain_g[0], shift_g[0])


def solution(mesh):
    placed = (
        P("dp", "sp", None),
        P("dp", "sp", None),
        P("dp", "sp", None),
        P(),
        P(),
        P("dp", None, None),
        P(),
    )
    return jax.shard_map(
        per_device,
        mesh=mesh,
        in_specs=placed,
        out_specs=(P("dp", "sp", None), P("dp", "sp", None), P("dp", None, None), P(), P(), P()),
        check_vma=False,
    )
```
